32 devices in a mesh: sp: 4 (over z), fs: 4 (over y, x), tp: 2 (over core).
Axes of the slice: x: 2, y: 2, z: 4, core: 2. Of those that a mesh axis runs over, the one named last changes fastest.
Arguments:
- tokens: bfloat16 [4, 1024, 2048], P('fs', ('sp', 'tp')), may hold values from -6 to 6
- norm_gain: float32 [2048], replicated, may hold values from 0.1 to 1.9
- w_query: bfloat16 [2048, 1024], P('fs', 'tp'), may hold values from -0.125 to 0.125
- w_key: bfloat16 [2048, 1024], P('fs', 'tp'), may hold values from -0.125 to 0.125
- w_value: bfloat16 [2048, 1024], P('fs', 'tp'), may hold values from -0.125 to 0.125
- w_conv_value: bfloat16 [2048, 1024], P('fs', 'tp'), may hold values from -2 to 2
- w_conv_gate: bfloat16 [2048, 1024], P('fs', 'tp'), may hold values from -0.125 to 0.125
- key_offset: bfloat16 [1024, 16], P('sp', 'tp'), may hold values from -16 to 2
- conv_kernel: float32 [31, 1024], P(None, 'tp'), may hold values from -3 to 3
- conv_gain: float32 [1024], P('tp'), may hold values from 0.1 to 1.9
- w_attn_out: bfloat16 [1024, 2048], P('tp', 'fs'), may hold values from -1 to 1
- w_conv_out: bfloat16 [1024, 2048], P('tp', 'fs'), may hold values from -0.1875 to 0.1875
Outputs:
- mixed: bfloat16 [4, 1024, 2048], P('fs', ('sp', 'tp'))
The draws below stay inside these ranges and needn't reach their ends.
All inputs are finite; a program needn't handle non-finite values.
Results may differ from the reference program's by a relative error of at most 0.0085.
Values may be sent and summed in bfloat16 or wider, within the bound.
A program may use at most 128 MiB of HBM per device.

```python
import math
import jax
import jax.numpy as jnp
from jax import lax

D = 2048
STICK_HEADS = 16
HD = 64
CC = 1024
KW = 31
TOK_DEV = 256
SBW = 1024
SEQUENCE_LENGTH = 1024
BATCH = 4
N_TP = 2


def draw_key_offset(key, part):
    divisions = jax.random.split(jax.random.fold_in(key, 11), 5)
    base_level = jax.random.uniform(divisions[0], (STICK_HEADS,), jnp.float32, -2.0, 5.0)
    block_shift = jax.random.uniform(divisions[1], (SEQUENCE_LENGTH // TOK_DEV, STICK_HEADS), jnp.float32, -0.8, 0.8)
    block_shift = jnp.repeat(block_shift, TOK_DEV, axis=0)
    roughness = jnp.clip(0.3 * jax.random.normal(divisions[2], (SEQUENCE_LENGTH, STICK_HEADS), jnp.float32), -1.0, 1.0)
    signal_height = base_level[None, :] - math.log(SEQUENCE_LENGTH) + block_shift + roughness
    spike_locations = jax.random.randint(divisions[3], (4,), 0, SEQUENCE_LENGTH)
    spike_flags = jnp.any(jnp.arange(SEQUENCE_LENGTH)[:, None] == spike_locations[None, :], axis=1)
    spike_magnitude = jax.random.uniform(divisions[4], (SEQUENCE_LENGTH, STICK_HEADS), jnp.float32, -1.2, 0.0)
    return jnp.where(spike_flags[:, None], spike_magnitude, signal_height).astype(jnp.bfloat16)


def draw_conv_kernel(key, part):
    divisions = jax.random.split(jax.random.fold_in(key, 23), 2)
    ramp = jnp.exp(jnp.linspace(math.log(0.4), math.log(2.0), CC)).astype(jnp.float32)
    entries = jnp.clip(jax.random.normal(divisions[0], (KW, CC), jnp.float32), -4.0, 4.0)
    common_tap = 0.1
    roughness = jax.random.uniform(divisions[1], (CC,), jnp.float32, 0.5, 1.5)
    return (entries * KW ** (-0.5) * ramp[None, :] * roughness[None, :] + common_tap).astype(jnp.float32)


def draw_w_conv_value(key, part):
    divisions = jax.random.split(jax.random.fold_in(key, 37), 3)
    levels = jnp.exp(jnp.linspace(math.log(0.3), math.log(3.0), CC)).astype(jnp.float32)
    noise = jnp.clip(jax.random.normal(divisions[0], (D, CC), jnp.float32), -4.0, 4.0)
    shared = jnp.clip(jax.random.normal(divisions[1], (D,), jnp.float32), -3.0, 3.0)
    roughness = jax.random.uniform(divisions[2], (CC,), jnp.float32, 0.7, 1.0)
    return ((noise + shared[:, None] * (levels * roughness)[None, :]) * D ** (-0.5)).astype(jnp.bfloat16)


def block_levels(stream_key, shape, pieces, smallest, top_value):
    def one(dim, blocks):
        heights = jax.random.uniform(jax.random.fold_in(jax.random.fold_in(stream_key, 6), dim), (blocks,), jnp.float32, smallest / len(pieces), top_value / len(pieces))
        return jnp.repeat(jnp.exp(heights), shape[dim] // blocks).reshape((-1,) + (1,) * (len(shape) - dim - 1))

    factor_of = one(*pieces[0])
    for cut in pieces[1:]:
        factor_of = factor_of * one(*cut)
    return factor_of


def bell_draw(own_key, extent, scale, limit, pieces=(), kind=jnp.bfloat16):
    gain = block_levels(own_key, extent, pieces, -0.22, 0.18) if pieces else 1.0
    values = jax.random.normal(own_key, extent, jnp.float32) * scale * gain
    return jnp.minimum(jnp.maximum(values, -limit), limit).astype(kind)


def setup_inputs(seed: int = 0) -> dict:
    streams_of = jax.random.split(jax.random.key(seed), 13)
    tokens = bell_draw(streams_of[0], (BATCH, SEQUENCE_LENGTH, D), 1.0, 6.0, ((0, 4), (1, 8)))
    norm_gain = jnp.clip(1.0 + 0.18 * jax.random.normal(streams_of[1], (D,), jnp.float32), 0.1, 1.9)
    w_query = bell_draw(streams_of[2], (D, SBW), D ** -0.5, 0.125, ((0, 4), (1, 2)))
    w_key = bell_draw(streams_of[3], (D, SBW), D ** -0.5, 0.125, ((0, 4), (1, 2)))
    w_value = bell_draw(streams_of[4], (D, SBW), D ** -0.5, 0.125, ((0, 4), (1, 2)))
    w_conv_value = draw_w_conv_value(jax.random.fold_in(streams_of[12], 71), 0)
    w_conv_gate = bell_draw(streams_of[6], (D, CC), D ** -0.5, 0.125, ((0, 4), (1, 2)))
    key_offset = draw_key_offset(jax.random.fold_in(streams_of[12], 71), 0)
    conv_kernel = draw_conv_kernel(jax.random.fold_in(streams_of[12], 71), 0)
    conv_gain = jnp.clip(1.0 + 0.18 * jax.random.normal(streams_of[9], (CC,), jnp.float32), 0.1, 1.9)
    w_attn_out = bell_draw(streams_of[10], (SBW, D), (SBW // 32) ** -0.5, 1.0, ((0, 2), (1, 4)))
    w_conv_out = bell_draw(streams_of[11], (CC, D), CC ** -0.5, 0.1875, ((0, 2), (1, 4)))
    return {"tokens": tokens, "norm_gain": norm_gain, "w_query": w_query, "w_key": w_key, "w_value": w_value, "w_conv_value": w_conv_value, "w_conv_gate": w_conv_gate, "key_offset": key_offset, "conv_kernel": conv_kernel, "conv_gain": conv_gain, "w_attn_out": w_attn_out, "w_conv_out": w_conv_out}


def reference(tokens, norm_gain, w_query, w_key, w_value, w_conv_value, w_conv_gate, key_offset, conv_kernel, conv_gain, w_attn_out, w_conv_out):
    floats = tokens.astype(jnp.float32)
    normed = (floats * lax.rsqrt(lax.optimization_barrier(jnp.mean(floats * floats, axis=2, keepdims=True)) + 1e-06) * norm_gain).astype(jnp.bfloat16)
    flat_rows = normed.reshape(BATCH * SEQUENCE_LENGTH, D)

    def project(weight):
        return jnp.dot(flat_rows, weight, preferred_element_type=jnp.float32).astype(jnp.bfloat16).reshape(BATCH, SEQUENCE_LENGTH, weight.shape[1])
    queries = project(w_query)
    key_rows = project(w_key)
    value_rows = project(w_value)
    conv_value = project(w_conv_value)
    conv_gate = project(w_conv_gate)
    offsets = jnp.transpose(key_offset.astype(jnp.float32))
    key_pos = jnp.arange(SEQUENCE_LENGTH, dtype=jnp.int32)
    blocks = SEQUENCE_LENGTH // TOK_DEV
    score_scale = HD ** (-0.5)

    def one_block(index):
        batch_index = index // blocks
        first_row = index % blocks * TOK_DEV
        seq_query = lax.dynamic_index_in_dim(queries, batch_index, 0, keepdims=False)
        query_block = lax.dynamic_slice_in_dim(seq_query, first_row, TOK_DEV, 0).reshape(TOK_DEV, STICK_HEADS, HD)
        seq_keys = lax.dynamic_index_in_dim(key_rows, batch_index, 0, keepdims=False).reshape(SEQUENCE_LENGTH, STICK_HEADS, HD)
        seq_values = lax.dynamic_index_in_dim(value_rows, batch_index, 0, keepdims=False).reshape(SEQUENCE_LENGTH, STICK_HEADS, HD)
        logits = jnp.einsum('qhd,khd->hqk', query_block.astype(jnp.float32), seq_keys.astype(jnp.float32)) * score_scale
        logits = logits + offsets[:, None, :]
        query_pos = first_row + jnp.arange(TOK_DEV, dtype=jnp.int32)
        allowed = key_pos[None, :] < query_pos[:, None]
        log_keep = jnp.where(allowed[None], jax.nn.log_sigmoid(-logits), 0.0)
        between = lax.cumsum(log_keep, axis=2, reverse=True) - log_keep
        weights = jnp.where(allowed[None], jnp.exp(jax.nn.log_sigmoid(logits) + between), 0.0).astype(jnp.bfloat16)
        result = jnp.einsum('hqk,khd->qhd', weights.astype(jnp.float32), seq_values.astype(jnp.float32))
        return result.reshape(TOK_DEV, SBW).astype(jnp.bfloat16)
    attn_heads = lax.map(one_block, jnp.arange(BATCH * blocks, dtype=jnp.int32)).reshape(BATCH, SEQUENCE_LENGTH, SBW)
    gated_input = (conv_value.astype(jnp.float32) * jax.nn.sigmoid(conv_gate.astype(jnp.float32))).astype(jnp.bfloat16)
    padded = jnp.pad(gated_input, ((0, 0), (KW - 1, 0), (0, 0))).astype(jnp.float32)
    conv_sum = jnp.zeros((BATCH, SEQUENCE_LENGTH, CC), jnp.float32)
    for tap_index in range(KW):
        conv_sum = conv_sum + conv_kernel[tap_index] * padded[:, tap_index:tap_index + SEQUENCE_LENGTH]
    mean_val = lax.optimization_barrier(jnp.mean(conv_sum, axis=2, keepdims=True))
    centred = conv_sum - mean_val
    spread = lax.optimization_barrier(jnp.mean(centred * centred, axis=2, keepdims=True))
    conv_hidden = jax.nn.silu(centred * lax.rsqrt(spread + 1e-06) * conv_gain).astype(jnp.bfloat16)
    head_cols = SBW // N_TP
    chan_cols = CC // N_TP
    attn_flat = attn_heads.reshape(BATCH * SEQUENCE_LENGTH, SBW)
    conv_flat = conv_hidden.reshape(BATCH * SEQUENCE_LENGTH, CC)
    total = jnp.zeros((BATCH * SEQUENCE_LENGTH, D), jnp.float32)
    for group in range(N_TP):
        partial_value = jnp.dot(attn_flat[:, group * head_cols:(group + 1) * head_cols], w_attn_out[group * head_cols:(group + 1) * head_cols], preferred_element_type=jnp.float32)
        partial_value = partial_value + jnp.dot(conv_flat[:, group * chan_cols:(group + 1) * chan_cols], w_conv_out[group * chan_cols:(group + 1) * chan_cols], preferred_element_type=jnp.float32)
        total = total + lax.optimization_barrier(partial_value.astype(jnp.bfloat16)).astype(jnp.float32)
    return total.astype(jnp.bfloat16).reshape(BATCH, SEQUENCE_LENGTH, D)
```

```python
import functools

import jax
import jax.numpy as jnp
from jax import lax
from jax.experimental import pallas as pl
from jax.experimental.pallas import tpu as pltpu
from jax.sharding import PartitionSpec as P

HD = 64
CC = 1024
MESH = pl.DeviceIdType.MESH
F32 = jnp.float32
BF16 = jnp.bfloat16


def remote(src, dst, send, recv, **where):
    return pltpu.make_async_remote_copy(
        src_ref=src, dst_ref=dst, send_sem=send, recv_sem=recv, device_id=where, device_id_type=MESH
    )


def greet(peers):
    barrier = pltpu.get_barrier_semaphore()
    for where in peers:
        pl.semaphore_signal(barrier, inc=1, device_id=where, device_id_type=MESH)
    pl.semaphore_wait(barrier, len(peers))


def plane(fs):
    y = (fs + 2) % 4
    return fs + 1 - 2 * (fs % 2), y, y + 1 - 2 * (y % 2)


class OutGather:
    def __init__(self, sources, targets, sems):
        self.sources, self.targets = sources, targets
        self.send, self.recv, self.psend, self.precv, self.local = sems
        self.fs, self.tp = lax.axis_index("fs"), lax.axis_index("tp")

    def slot(self, k, owner, group):
        rows, cols = self.sources[k].shape
        return self.targets[k].at[
            pl.ds(pl.multiple_of(group * rows, rows), rows),
            pl.ds(pl.multiple_of(owner * cols, cols), cols),
        ]

    def hop(self, src, k, owner, sem, to):
        return remote(src, self.slot(k, owner, self.tp), self.send.at[sem], self.recv.at[sem], fs=to)

    def other(self, src, k, owner, sem):
        return remote(
            src, self.slot(k, owner, self.tp), self.psend.at[sem], self.precv.at[sem], tp=1 - self.tp
        )

    def plan(self):
        fs = self.fs
        xn, yn, dg = plane(fs)
        a, c = self.sources
        self.first = [
            self.hop(a, 0, fs, 0, xn), self.hop(c, 1, fs, 1, yn),
            self.hop(c, 1, fs, 2, xn), self.hop(a, 0, fs, 3, yn),
        ]
        self.relay = [
            self.hop(self.slot(0, xn, self.tp), 0, xn, 4, yn),
            self.hop(self.slot(1, yn, self.tp), 1, yn, 5, xn),
        ]
        arrivals = [(0, 0, xn), (1, 1, yn), (2, 1, xn), (3, 0, yn), (4, 0, dg), (5, 1, dg)]
        self.got = [
            (self.hop(self.slot(k, o, self.tp), k, o, s, xn), self.other(self.slot(k, o, self.tp), k, o, s))
            for s, k, o in arrivals
        ]
        self.own = [self.other(a, 0, fs, 6), self.other(c, 1, fs, 7)]
        self.keep = [
            pltpu.make_async_copy(self.sources[k], self.slot(k, fs, self.tp), self.local.at[k]) for k in (0, 1)
        ]

    def start(self):
        self.plan()
        for copy in self.first + self.own + self.keep:
            copy.start()

    def middle(self):
        for s in range(4):
            arrived, onward = self.got[s]
            arrived.wait_recv()
            if s < 2:
                self.relay[s].start()
            onward.start()

    def finish(self):
        for s in (4, 5):
            arrived, onward = self.got[s]
            arrived.wait_recv()
            onward.start()
        for copy in self.first + self.relay:
            copy.wait_send()
        for _, onward in self.got:
            onward.wait()
        for copy in self.own:
            copy.wait()
        for copy in self.keep:
            copy.wait()


OUT_SEMS = [
    pltpu.SemaphoreType.DMA((6,)),
    pltpu.SemaphoreType.DMA((6,)),
    pltpu.SemaphoreType.DMA((8,)),
    pltpu.SemaphoreType.DMA((8,)),
    pltpu.SemaphoreType.DMA((2,)),
]


def gather_kernel(n_sp, with_out, *refs):
    tok, w_ins, off = refs[0], refs[1:6], refs[6]
    refs = refs[7:]
    if with_out:
        out_sources, refs = refs[:2], refs[2:]
    tok_all, w_all, off_all = refs[:3]
    refs = refs[3:]
    if with_out:
        out_targets, refs = refs[:2], refs[2:]
    stage, up_s, up_r, dn_s, dn_r, par_s, par_r, w_s, w_r, off_s, off_r, loc = refs[:12]
    z, fs, tp = lax.axis_index("sp"), lax.axis_index("fs"), lax.axis_index("tp")
    xn, yn, dg = plane(fs)
    rows = w_ins[0].shape[0]
    width = stage.shape[1] // 5
    half = rows // 2

    fills = [
        pltpu.make_async_copy(
            w.at[:, pl.ds(pl.multiple_of(z * width, width), width)],
            stage.at[:, pl.ds(k * width, width)],
            loc.at[k],
        )
        for k, w in enumerate(w_ins)
    ]
    for fill in fills:
        fill.start()
    keep_tok = pltpu.make_async_copy(tok, tok_all.at[z, tp], loc.at[5])
    keep_off = pltpu.make_async_copy(off, off_all.at[z], loc.at[6])
    keep_tok.start()
    keep_off.start()
    greet(
        [{"sp": (z + d) % n_sp} for d in range(1, n_sp)]
        + [{"fs": xn}, {"fs": yn}, {"tp": 1 - tp}]
    )

    def lift(src, block, dist):
        return remote(src, tok_all.at[block, tp], up_s.at[dist - 1], up_r.at[dist - 1], sp=(z + 1) % n_sp)

    def sink(src, block, dist):
        return remote(src, tok_all.at[block, tp], dn_s.at[dist - 1], dn_r.at[dist - 1], sp=(z + n_sp - 1) % n_sp)

    def across(src, block):
        return remote(src, tok_all.at[block, tp], par_s.at[block], par_r.at[block], tp=1 - tp)

    @pl.when(z < n_sp - 1)
    def _():
        lift(tok, z, 1).start()

    @pl.when(z > 0)
    def _():
        sink(tok, z, 1).start()

    across(tok, z).start()
    offs = [
        remote(off, off_all.at[z], off_s.at[d - 1], off_r.at[d - 1], sp=(z + d) % n_sp) for d in range(1, n_sp)
    ]
    for copy in offs:
        copy.start()
    for fill in fills:
        fill.wait()
    keep_w = pltpu.make_async_copy(stage, w_all.at[pl.ds(pl.multiple_of(fs * rows, rows), rows)], loc.at[7])
    keep_w.start()

    def part(owner, h):
        return w_all.at[pl.ds(pl.multiple_of(owner * rows + h * half, half), half)]

    def send_w(src, owner, h, sem, to):
        return remote(src, part(owner, h), w_s.at[sem], w_r.at[sem], fs=to)

    own = [stage.at[pl.ds(h * half, half)] for h in range(2)]
    first = [
        send_w(own[0], fs, 0, 0, xn), send_w(own[1], fs, 1, 1, yn),
        send_w(own[1], fs, 1, 2, xn), send_w(own[0], fs, 0, 3, yn),
    ]
    for copy in first:
        copy.start()
    relay = [send_w(part(xn, 0), xn, 0, 4, yn), send_w(part(yn, 1), yn, 1, 5, xn)]
    if with_out:
        gather = OutGather(out_sources, out_targets, refs[12:])
    arrivals = [(0, xn, 0), (1, yn, 1), (2, xn, 1), (3, yn, 0), (4, dg, 0), (5, dg, 1)]
    for s, owner, h in arrivals[:2]:
        send_w(part(owner, h), owner, h, s, xn).wait_recv()
        relay[s].start()
    if with_out:
        gather.start()

    for dist in range(1, n_sp):
        @pl.when(z >= dist)
        def _():
            block = (z - dist + n_sp) % n_sp
            lift(tok_all.at[block, tp], block, dist).wait_recv()
            if dist < n_sp - 1:
                @pl.when(z < n_sp - 1)
                def _():
                    lift(tok_all.at[block, tp], block, dist + 1).start()
            across(tok_all.at[block, tp], block).start()

        @pl.when(z + dist < n_sp)
        def _():
            block = (z + dist) % n_sp
            sink(tok_all.at[block, tp], block, dist).wait_recv()
            if dist < n_sp - 1:
                @pl.when(z > 0)
                def _():
                    sink(tok_all.at[block, tp], block, dist + 1).start()
            across(tok_all.at[block, tp], block).start()

    for s, owner, h in arrivals[2:]:
        send_w(part(owner, h), owner, h, s, xn).wait_recv()
    if with_out:
        gather.middle()
        gather.finish()
    for copy in first + relay:
        copy.wait_send()
    for dist in range(1, n_sp):
        @pl.when(jnp.logical_and(z < n_sp - 1, z >= dist - 1))
        def _():
            lift(tok, z, dist).wait_send()

        @pl.when(jnp.logical_and(z > 0, z + dist - 1 < n_sp))
        def _():
            sink(tok, z, dist).wait_send()

    for block in range(n_sp):
        remote(tok, tok_all.at[block, 1 - tp], par_s.at[block], par_r.at[block], tp=1 - tp).wait()
    for copy in offs:
        copy.wait()
    keep_tok.wait()
    keep_off.wait()
    keep_w.wait()


ANY = pl.BlockSpec(memory_space=pl.ANY)
VMEM = pl.BlockSpec(memory_space=pltpu.VMEM)


def gather_call(n_sp, n_fs, n_tp, width, tokens, w_ins, offsets, w_outs):
    rows, features = tokens.shape
    depth = w_ins[0].shape[0]
    o_rows, o_cols = w_outs[0].shape
    dma = pltpu.SemaphoreType.DMA
    return pl.pallas_call(
        functools.partial(gather_kernel, n_sp, True),
        out_shape=[
            jax.ShapeDtypeStruct((n_sp, n_tp, rows, features), BF16),
            jax.ShapeDtypeStruct((n_fs * depth, 5 * width), BF16),
            jax.ShapeDtypeStruct((n_sp,) + offsets.shape, F32),
            jax.ShapeDtypeStruct((n_tp * o_rows, n_fs * o_cols), BF16),
            jax.ShapeDtypeStruct((n_tp * o_rows, n_fs * o_cols), BF16),
        ],
        in_specs=[ANY] * 9,
        out_specs=[ANY] * 5,
        scratch_shapes=[
            pltpu.VMEM((depth, 5 * width), BF16),
            dma((n_sp - 1,)), dma((n_sp - 1,)), dma((n_sp - 1,)), dma((n_sp - 1,)),
            dma((n_sp,)), dma((n_sp,)),
            dma((6,)), dma((6,)),
            dma((n_sp - 1,)), dma((n_sp - 1,)),
            dma((8,)),
        ] + OUT_SEMS,
        compiler_params=pltpu.CompilerParams(collective_id=0, has_side_effects=True),
        name="gather_inputs",
    )(tokens, *w_ins, offsets, *w_outs)


def compute_body(width, heads, taps, blk, tok, gain, w, off, ck, attn_out, conv_out, mean_out, proj, gated):
    length = tok.shape[0]
    n_rows = mean_out.shape[2]

    def project(i, _):
        at = pl.ds(pl.multiple_of(i * 128, 128), 128)
        x = tok[at, :].astype(F32)
        normed = (x * lax.rsqrt(jnp.mean(x * x, axis=1, keepdims=True) + 1e-06) * gain[...]).astype(BF16)
        out = jnp.dot(normed, w[...], preferred_element_type=F32).astype(BF16)
        proj[at, :] = out[:, : 3 * width]
        value = out[:, 3 * width : 4 * width].astype(F32)
        gate = out[:, 4 * width :].astype(F32)
        gated[pl.ds(pl.multiple_of(i * 128 + 32, 32), 128), :] = (value * jax.nn.sigmoid(gate)).astype(BF16).astype(F32)
        return 0

    gated[pl.ds(0, 32), :] = jnp.zeros((32, width), F32)
    lax.fori_loop(0, length // 128, project, 0)

    ones = jnp.full((8, width), 1.0 / width, F32)

    def convolve(i, _):
        base = pl.multiple_of(i * n_rows, n_rows)
        window = gated[pl.ds(base, n_rows + 32), :]
        total = jnp.zeros((n_rows, width), F32)
        for tap in range(taps):
            lo = 32 - (taps - 1) + tap
            total = total + ck[tap : tap + 1, :] * window[lo : lo + n_rows]
        local = jnp.mean(total, axis=1, keepdims=True)
        conv_out[pl.ds(base, n_rows), :] = (total - local).astype(BF16)
        mean_out[i] = lax.dot_general(
            ones, total, (((1,), (1,)), ((), ())), precision=lax.Precision.HIGHEST, preferred_element_type=F32
        )
        return 0

    lax.fori_loop(0, length // n_rows, convolve, 0)

    row = lax.broadcasted_iota(jnp.int32, (blk, blk), 0)
    col = lax.broadcasted_iota(jnp.int32, (blk, blk), 1)
    allowed = col < row
    after = jnp.where(row >= col, 1.0, 0.0).astype(BF16)
    lane = lax.broadcasted_iota(jnp.int32, (blk, width), 1)

    def attend(i, _):
        q_at = pl.ds(pl.multiple_of(i * blk, blk), blk)
        merged = jnp.zeros((blk, width), F32)
        for h in range(heads):
            mine = jnp.logical_and(lane >= h * HD, lane < (h + 1) * HD)
            q = jnp.where(mine, proj[q_at, :width].astype(F32) * HD ** (-0.5), 0.0).astype(BF16)

            def piece(j, carry, total, diagonal):
                k_at = pl.ds(pl.multiple_of(j * blk, blk), blk)
                k = proj[k_at, width : 2 * width]
                v = proj[k_at, 2 * width : 3 * width]
                s = lax.dot_general(q, k, (((1,), (1,)), ((), ())), preferred_element_type=F32)
                s = s + off[j, h : h + 1, :]
                keep = -(jnp.maximum(s, 0.0) + jnp.log(1.0 + jnp.exp(-jnp.abs(s))))
                if diagonal:
                    keep = jnp.where(allowed, keep, 0.0)
                high = keep.astype(BF16)
                low = (keep - high.astype(F32)).astype(BF16)
                suffix = jnp.dot(high, after, preferred_element_type=F32)
                suffix = suffix + jnp.dot(low, after, preferred_element_type=F32)
                weights = jnp.exp(s + suffix + carry)
                if diagonal:
                    weights = jnp.where(allowed, weights, 0.0)
                total = total + jnp.dot(weights.astype(BF16), v, preferred_element_type=F32)
                return carry + suffix[:, :1], total

            carry, total = piece(i, jnp.zeros((blk, 1), F32), jnp.zeros((blk, width), F32), True)
            carry, total = lax.fori_loop(
                0, i, lambda t, c: piece(i - 1 - t, c[0], c[1], False), (carry, total)
            )
            merged = jnp.where(mine, total, merged)
        attn_out[q_at, :] = merged.astype(BF16)
        return 0

    lax.fori_loop(0, length // blk, attend, 0)


def compute_call(width, heads, blk, n_dest, tok, gain, w, off, ck):
    length = tok.shape[0]
    return pl.pallas_call(
        functools.partial(compute_body, width, heads, ck.shape[0], blk),
        out_shape=[
            jax.ShapeDtypeStruct((length, width), BF16),
            jax.ShapeDtypeStruct((length, width), BF16),
            jax.ShapeDtypeStruct((n_dest, 8, length // n_dest), F32),
        ],
        in_specs=[VMEM] * 5,
        out_specs=[VMEM] * 3,
        scratch_shapes=[pltpu.VMEM((length, 3 * width), BF16), pltpu.VMEM((length + 32, width), F32)],
        name="branches",
    )(tok, gain, w, off, ck)


def exchange_kernel(n_sp, n_tp, attn, conv, mean, x_out, mean_all, send, recv, loc):
    z, tp = lax.axis_index("sp"), lax.axis_index("tp")
    me = z * n_tp + tp
    n = n_sp * n_tp
    rows, cols = x_out.shape
    width = attn.shape[1]
    place = tp * n_sp + z

    def slots(index):
        return (
            x_out.at[:, pl.ds(pl.multiple_of(index * width, width), width)],
            x_out.at[:, pl.ds(pl.multiple_of(cols // 2 + index * width, width), width)],
            mean_all.at[index],
        )

    def pieces(dest):
        at = pl.ds(pl.multiple_of(dest * rows, rows), rows)
        return (attn.at[at], conv.at[at], mean.at[dest])

    keeps = [
        pltpu.make_async_copy(s, d, loc.at[k]) for k, (s, d) in enumerate(zip(pieces(me), slots(place)))
    ]
    for copy in keeps:
        copy.start()
    peers = [(me + d) % n for d in range(1, n)]
    greet([{"sp": p // n_tp, "tp": p % n_tp} for p in peers])
    copies = []
    for d, p in enumerate(peers):
        for k, (s, t) in enumerate(zip(pieces(p), slots(place))):
            copies.append(remote(s, t, send.at[d, k], recv.at[d, k], sp=p // n_tp, tp=p % n_tp))
    for copy in copies:
        copy.start()
    for d in range(1, n):
        src = (me - d + n) % n
        for k, (s, t) in enumerate(zip(pieces(me), slots((src % n_tp) * n_sp + src // n_tp))):
            remote(s, t, send.at[d - 1, k], recv.at[d - 1, k], sp=z, tp=1 - tp).wait_recv()
    for copy in copies:
        copy.wait_send()
    for copy in keeps:
        copy.wait()


def exchange_call(n_sp, n_tp, attn, conv, mean):
    n = n_sp * n_tp
    length, width = attn.shape
    dma = pltpu.SemaphoreType.DMA
    return pl.pallas_call(
        functools.partial(exchange_kernel, n_sp, n_tp),
        out_shape=[
            jax.ShapeDtypeStruct((length // n, 2 * width * n), BF16),
            jax.ShapeDtypeStruct((n, 8, length // n), F32),
        ],
        in_specs=[VMEM] * 3,
        out_specs=[VMEM] * 2,
        scratch_shapes=[dma((n - 1, 3)), dma((n - 1, 3)), dma((3,))],
        compiler_params=pltpu.CompilerParams(collective_id=1, has_side_effects=True),
        name="to_positions",
    )(attn, conv, mean)


def spread_shards(
    tokens,
    norm_gain,
    w_query,
    w_key,
    w_value,
    w_conv_value,
    w_conv_gate,
    key_offset,
    conv_kernel,
    conv_gain,
    w_attn_out,
    w_conv_out,
):
    n_sp, n_fs, n_tp = (lax.axis_size(a) for a in ("sp", "fs", "tp"))
    z, tp = lax.axis_index("sp"), lax.axis_index("tp")
    width = w_query.shape[1] // n_sp
    heads = width // HD
    offsets = jnp.transpose(key_offset.astype(F32))
    tok_all, w_all, off_all, wa, wc = gather_call(
        n_sp, n_fs, n_tp, width, tokens[0],
        (w_query, w_key, w_value, w_conv_value, w_conv_gate), offsets, (w_attn_out, w_conv_out),
    )
    features = tokens.shape[2]
    tok_all = tok_all.reshape(-1, features)
    off = lax.dynamic_slice_in_dim(off_all, z * heads, heads, axis=1)
    taps = lax.dynamic_slice_in_dim(conv_kernel, z * width, width, axis=1)
    attn, conv, mean = compute_call(
        width, heads, key_offset.shape[0], n_sp * n_tp, tok_all, norm_gain[None], w_all, off, taps
    )
    x, means = exchange_call(n_sp, n_tp, attn, conv, mean)
    half = x.shape[1] // 2
    groups = n_sp * n_tp
    local = jnp.transpose(means[:, 0, :])
    local = local - jnp.mean(local, axis=1, keepdims=True)
    gain = lax.all_gather(conv_gain, "tp", axis=0, tiled=True)
    centred = (x[:, half:].astype(F32).reshape(-1, groups, width) + local[:, :, None]).reshape(-1, half)
    centred = centred - jnp.mean(centred, axis=1, keepdims=True)
    spread = jnp.mean(centred * centred, axis=1, keepdims=True)
    hidden = jax.nn.silu(centred * lax.rsqrt(spread + 1e-06) * gain).astype(BF16)
    mixed = jnp.dot(x[:, :half], wa, preferred_element_type=F32)
    mixed = mixed + jnp.dot(hidden, wc, preferred_element_type=F32)
    return mixed.astype(BF16)[None]


def shifted(block, axis, distance):
    devices = range(lax.axis_size(axis))
    route = [(i - distance, i) for i in devices if i - distance in devices]
    return lax.ppermute(block, axis, route)


def piece_terms(queries, key_rows, value_rows, offsets, carry_log, allowed):
    head_size = queries.shape[2]
    logits = jnp.einsum(
        "qhd,khd->hqk", queries, key_rows, preferred_element_type=jnp.float32
    ) * head_size ** (-0.5)
    logits = logits + jnp.transpose(offsets.astype(jnp.float32))[:, None, :]
    log_keep = jax.nn.log_sigmoid(-logits)
    if allowed is not None:
        log_keep = jnp.where(allowed[None], log_keep, 0.0)
    between = lax.cumsum(log_keep, axis=2, reverse=True) - log_keep
    weights = jnp.exp(jax.nn.log_sigmoid(logits) + between + carry_log[:, :, None])
    if allowed is not None:
        weights = jnp.where(allowed[None], weights, 0.0)
    result = jnp.einsum(
        "hqk,khd->qhd", weights.astype(jnp.bfloat16), value_rows, preferred_element_type=jnp.float32
    )
    return (result, carry_log + jnp.sum(log_keep, axis=2))


def shards(
    tokens,
    norm_gain,
    w_query,
    w_key,
    w_value,
    w_conv_value,
    w_conv_gate,
    key_offset,
    conv_kernel,
    conv_gain,
    w_attn_out,
    w_conv_out,
):
    gathered = (
        lax.all_gather(w_query, "fs", axis=0, tiled=True),
        lax.all_gather(w_key, "fs", axis=0, tiled=True),
        lax.all_gather(w_value, "fs", axis=0, tiled=True),
        lax.all_gather(w_conv_value, "fs", axis=0, tiled=True),
        lax.all_gather(w_conv_gate, "fs", axis=0, tiled=True),
    )
    floats = lax.all_gather(tokens[0], "tp", axis=0, tiled=True).astype(jnp.float32)
    normed = (
        floats * lax.rsqrt(jnp.mean(floats * floats, axis=1, keepdims=True) + 1e-06) * norm_gain
    ).astype(jnp.bfloat16)
    projected = jnp.concatenate(
        [
            jnp.dot(normed, weight, preferred_element_type=jnp.float32).astype(jnp.bfloat16)
            for weight in gathered
        ],
        axis=1,
    )
    head_cols = w_query.shape[1]
    channels = w_conv_value.shape[1]
    block_len = projected.shape[0]
    local_heads = head_cols // HD
    queries = projected[:, :head_cols].reshape(block_len, local_heads, HD)
    key_flat = projected[:, head_cols : 2 * head_cols]
    value_flat = projected[:, 2 * head_cols : 3 * head_cols]
    conv_value = projected[:, 3 * head_cols : 3 * head_cols + channels]
    conv_gate = projected[:, 3 * head_cols + channels :]
    position = lax.axis_index("sp")
    positions = jnp.arange(block_len, dtype=jnp.int32)
    causal = positions[None, :] < positions[:, None]
    start_log = jnp.zeros((local_heads, block_len), jnp.float32)
    totals, carry_log = piece_terms(
        queries,
        key_flat.reshape(block_len, local_heads, HD),
        value_flat.reshape(block_len, local_heads, HD),
        key_offset,
        start_log,
        causal,
    )

    def visit(hop_count, carried):
        running, running_log, moving = carried
        moving = shifted((moving[0], moving[1], moving[2]), "sp", 1)
        result, next_log = piece_terms(
            queries,
            moving[0].reshape(block_len, local_heads, HD),
            moving[1].reshape(block_len, local_heads, HD),
            moving[2],
            running_log,
            None,
        )
        active = position >= hop_count
        running = jnp.where(active, running + result, running)
        running_log = jnp.where(active, next_log, running_log)
        return (running, running_log, moving)

    totals, carry_log, leftover = lax.fori_loop(
        1, lax.axis_size("sp"), visit, (totals, carry_log, (key_flat, value_flat, key_offset))
    )
    attn_heads = totals.reshape(block_len, head_cols).astype(jnp.bfloat16)
    gated_input = (
        conv_value.astype(jnp.float32) * jax.nn.sigmoid(conv_gate.astype(jnp.float32))
    ).astype(jnp.bfloat16)
    kernel_len = conv_kernel.shape[0]
    edge_rows = shifted(gated_input[block_len - (kernel_len - 1) :], "sp", 1)
    extended = jnp.concatenate([edge_rows, gated_input], axis=0).astype(jnp.float32)
    conv_sum = jnp.zeros((block_len, channels), jnp.float32)
    for tap_index in range(kernel_len):
        conv_sum = conv_sum + conv_kernel[tap_index] * extended[tap_index : tap_index + block_len]
    channel_total = lax.psum(jnp.sum(conv_sum, axis=1), "tp")
    centred = conv_sum - (channel_total / CC)[:, None]
    spread = lax.psum(jnp.sum(centred * centred, axis=1), "tp") / CC
    conv_hidden = jax.nn.silu(centred * lax.rsqrt(spread + 1e-06)[:, None] * conv_gain).astype(
        jnp.bfloat16
    )
    attn_weight, conv_weight = (
        lax.all_gather(w_attn_out, "fs", axis=1, tiled=True),
        lax.all_gather(w_conv_out, "fs", axis=1, tiled=True),
    )
    partial_value = jnp.dot(attn_heads, attn_weight, preferred_element_type=jnp.float32)
    partial_value = partial_value + jnp.dot(
        conv_hidden, conv_weight, preferred_element_type=jnp.float32
    )
    mixed = lax.psum_scatter(
        lax.optimization_barrier(partial_value.astype(jnp.bfloat16))
        .astype(jnp.float32)
        .astype(jnp.bfloat16),
        "tp",
        scatter_dimension=0,
        tiled=True,
    )
    return mixed[None]


def solution(mesh):
    placed = (
        P("fs", ("sp", "tp"), None),
        P(),
        P("fs", "tp"),
        P("fs", "tp"),
        P("fs", "tp"),
        P("fs", "tp"),
        P("fs", "tp"),
        P("sp", "tp"),
        P(None, "tp"),
        P("tp"),
        P("tp", "fs"),
        P("tp", "fs"),
    )

    def fits(tokens, norm_gain, w_query, *rest):
        n_sp, n_fs, n_tp = mesh.shape["sp"], mesh.shape["fs"], mesh.shape["tp"]
        cols = w_query.shape[1] // n_tp
        return n_fs == 4 and n_tp == 2 and n_sp > 1 and rest[5].shape[0] <= 33 and cols % (128 * n_sp) == 0 and rest[2].shape[1] == w_query.shape[1] and (
            tokens.shape[1] % (128 * n_sp * n_tp) == 0
        )

    def program(*args):
        body = spread_shards if fits(*args) else shards
        return mapped(body)(*args)

    def mapped(body):
        return jax.shard_map(
            body, mesh=mesh, in_specs=placed, out_specs=P("fs", ("sp", "tp"), None), check_vma=False
        )

    return program
```

```python
import functools

import jax
import jax.numpy as jnp
from jax import lax
from jax.experimental import pallas as pl
from jax.experimental.pallas import tpu as pltpu
from jax.sharding import PartitionSpec as P

HD = 64
CC = 1024
MESH = pl.DeviceIdType.MESH
F32 = jnp.float32
BF16 = jnp.bfloat16


def remote(src, dst, send, recv, **where):
    return pltpu.make_async_remote_copy(
        src_ref=src, dst_ref=dst, send_sem=send, recv_sem=recv, device_id=where, device_id_type=MESH
    )


def greet(peers):
    barrier = pltpu.get_barrier_semaphore()
    for where in peers:
        pl.semaphore_signal(barrier, inc=1, device_id=where, device_id_type=MESH)
    pl.semaphore_wait(barrier, len(peers))


def plane(fs):
    y = (fs + 2) % 4
    return fs + 1 - 2 * (fs % 2), y, y + 1 - 2 * (y % 2)


class OutGather:
    def __init__(self, source, target, sems):
        half = source.shape[0] // 2
        self.sources = [source.at[pl.ds(k * half, half)] for k in range(2)]
        self.target = target
        self.send, self.recv, self.psend, self.precv, self.local = sems
        self.fs, self.tp = lax.axis_index("fs"), lax.axis_index("tp")

    def slot(self, k, owner, group):
        rows, cols = self.sources[k].shape
        return self.target.at[
            pl.ds(pl.multiple_of((group * 2 + k) * rows, rows), rows),
            pl.ds(pl.multiple_of(owner * cols, cols), cols),
        ]

    def hop(self, src, k, owner, sem, to):
        return remote(src, self.slot(k, owner, self.tp), self.send.at[sem], self.recv.at[sem], fs=to)

    def other(self, src, k, owner, sem):
        return remote(
            src, self.slot(k, owner, self.tp), self.psend.at[sem], self.precv.at[sem], tp=1 - self.tp
        )

    def plan(self):
        fs = self.fs
        xn, yn, dg = plane(fs)
        a, c = self.sources
        self.first = [
            self.hop(a, 0, fs, 0, xn), self.hop(c, 1, fs, 1, yn),
            self.hop(c, 1, fs, 2, xn), self.hop(a, 0, fs, 3, yn),
        ]
        self.relay = [
            self.hop(self.slot(0, xn, self.tp), 0, xn, 4, yn),
            self.hop(self.slot(1, yn, self.tp), 1, yn, 5, xn),
        ]
        arrivals = [(0, 0, xn), (1, 1, yn), (2, 1, xn), (3, 0, yn), (4, 0, dg), (5, 1, dg)]
        self.got = [
            (self.hop(self.slot(k, o, self.tp), k, o, s, xn), self.other(self.slot(k, o, self.tp), k, o, s))
            for s, k, o in arrivals
        ]
        self.own = [self.other(a, 0, fs, 6), self.other(c, 1, fs, 7)]
        self.keep = [
            pltpu.make_async_copy(self.sources[k], self.slot(k, fs, self.tp), self.local.at[k]) for k in (0, 1)
        ]

    def start(self):
        self.plan()
        for copy in self.first + self.own + self.keep:
            copy.start()

    def middle(self):
        for s in range(4):
            arrived, onward = self.got[s]
            arrived.wait_recv()
            if s < 2:
                self.relay[s].start()
            onward.start()

    def finish(self):
        for s in (4, 5):
            arrived, onward = self.got[s]
            arrived.wait_recv()
            onward.start()
        for copy in self.first + self.relay:
            copy.wait_send()
        for _, onward in self.got:
            onward.wait()
        for copy in self.own:
            copy.wait()
        for copy in self.keep:
            copy.wait()


OUT_SEMS = [
    pltpu.SemaphoreType.DMA((6,)),
    pltpu.SemaphoreType.DMA((6,)),
    pltpu.SemaphoreType.DMA((8,)),
    pltpu.SemaphoreType.DMA((8,)),
    pltpu.SemaphoreType.DMA((2,)),
]


def gather_kernel(n_sp, with_out, *refs):
    tok, w_ins, off = refs[0], refs[1:6], refs[6]
    refs = refs[7:]
    if with_out:
        out_source, cgain, refs = refs[0], refs[1], refs[2:]
    tok_all, w_all, off_all = refs[:3]
    refs = refs[3:]
    if with_out:
        out_target, cgain_all, refs = refs[0], refs[1], refs[2:]
    stage, up_s, up_r, dn_s, dn_r, par_s, par_r, w_s, w_r, off_s, off_r, loc = refs[:12]
    z, fs, tp = lax.axis_index("sp"), lax.axis_index("fs"), lax.axis_index("tp")
    xn, yn, dg = plane(fs)
    rows = w_ins[0].shape[0]
    width = stage.shape[1] // 5
    half = rows // 2

    fills = [
        pltpu.make_async_copy(
            w.at[:, pl.ds(pl.multiple_of(z * width, width), width)],
            stage.at[:, pl.ds(k * width, width)],
            loc.at[k],
        )
        for k, w in enumerate(w_ins)
    ]
    for fill in fills:
        fill.start()
    keep_tok = pltpu.make_async_copy(tok, tok_all.at[z, tp], loc.at[5])
    keep_off = pltpu.make_async_copy(off, off_all.at[z], loc.at[6])
    keep_gain = pltpu.make_async_copy(cgain, cgain_all.at[tp], loc.at[8])
    keep_tok.start()
    keep_off.start()
    keep_gain.start()
    greet(
        [{"sp": (z + d) % n_sp} for d in range(1, n_sp)]
        + [{"fs": xn}, {"fs": yn}, {"tp": 1 - tp}]
    )

    def lift(src, block, dist):
        return remote(src, tok_all.at[block, tp], up_s.at[dist - 1], up_r.at[dist - 1], sp=(z + 1) % n_sp)

    def sink(src, block, dist):
        return remote(src, tok_all.at[block, tp], dn_s.at[dist - 1], dn_r.at[dist - 1], sp=(z + n_sp - 1) % n_sp)

    def across(src, block):
        return remote(src, tok_all.at[block, tp], par_s.at[block], par_r.at[block], tp=1 - tp)

    @pl.when(z < n_sp - 1)
    def _():
        lift(tok, z, 1).start()

    @pl.when(z > 0)
    def _():
        sink(tok, z, 1).start()

    across(tok, z).start()
    offs = [
        remote(off, off_all.at[z], off_s.at[d - 1], off_r.at[d - 1], sp=(z + d) % n_sp) for d in range(1, n_sp)
    ]
    gain_copy = remote(cgain, cgain_all.at[tp], refs[17].at[0], refs[17].at[1], tp=1 - tp)
    gain_copy.start()
    for copy in offs:
        copy.start()
    for fill in fills:
        fill.wait()
    keep_w = pltpu.make_async_copy(stage, w_all.at[pl.ds(pl.multiple_of(fs * rows, rows), rows)], loc.at[7])
    keep_w.start()

    def part(owner, h):
        return w_all.at[pl.ds(pl.multiple_of(owner * rows + h * half, half), half)]

    def send_w(src, owner, h, sem, to):
        return remote(src, part(owner, h), w_s.at[sem], w_r.at[sem], fs=to)

    own = [stage.at[pl.ds(h * half, half)] for h in range(2)]
    first = [
        send_w(own[0], fs, 0, 0, xn), send_w(own[1], fs, 1, 1, yn),
        send_w(own[1], fs, 1, 2, xn), send_w(own[0], fs, 0, 3, yn),
    ]
    for copy in first:
        copy.start()
    relay = [send_w(part(xn, 0), xn, 0, 4, yn), send_w(part(yn, 1), yn, 1, 5, xn)]
    if with_out:
        gather = OutGather(out_source, out_target, refs[12:17])
    arrivals = [(0, xn, 0), (1, yn, 1), (2, xn, 1), (3, yn, 0), (4, dg, 0), (5, dg, 1)]
    for s, owner, h in arrivals[:2]:
        send_w(part(owner, h), owner, h, s, xn).wait_recv()
        relay[s].start()
    if with_out:
        gather.start()

    for dist in range(1, n_sp):
        @pl.when(z >= dist)
        def _():
            block = (z - dist + n_sp) % n_sp
            lift(tok_all.at[block, tp], block, dist).wait_recv()
            if dist < n_sp - 1:
                @pl.when(z < n_sp - 1)
                def _():
                    lift(tok_all.at[block, tp], block, dist + 1).start()
            across(tok_all.at[block, tp], block).start()

        @pl.when(z + dist < n_sp)
        def _():
            block = (z + dist) % n_sp
            sink(tok_all.at[block, tp], block, dist).wait_recv()
            if dist < n_sp - 1:
                @pl.when(z > 0)
                def _():
                    sink(tok_all.at[block, tp], block, dist + 1).start()
            across(tok_all.at[block, tp], block).start()

    for s, owner, h in arrivals[2:]:
        send_w(part(owner, h), owner, h, s, xn).wait_recv()
    if with_out:
        gather.middle()
        gather.finish()
    for copy in first + relay:
        copy.wait_send()
    for dist in range(1, n_sp):
        @pl.when(jnp.logical_and(z < n_sp - 1, z >= dist - 1))
        def _():
            lift(tok, z, dist).wait_send()

        @pl.when(jnp.logical_and(z > 0, z + dist - 1 < n_sp))
        def _():
            sink(tok, z, dist).wait_send()

    for block in range(n_sp):
        remote(tok, tok_all.at[block, 1 - tp], par_s.at[block], par_r.at[block], tp=1 - tp).wait()
    for copy in offs:
        copy.wait()
    gain_copy.wait()
    keep_gain.wait()
    keep_tok.wait()
    keep_off.wait()
    keep_w.wait()


ANY = pl.BlockSpec(memory_space=pl.ANY)
VMEM = pl.BlockSpec(memory_space=pltpu.VMEM)


def gather_call(n_sp, n_fs, n_tp, width, tokens, w_ins, offsets, w_out, conv_gain):
    rows, features = tokens.shape
    depth = w_ins[0].shape[0]
    o_rows, o_cols = w_out.shape
    dma = pltpu.SemaphoreType.DMA
    return pl.pallas_call(
        functools.partial(gather_kernel, n_sp, True),
        out_shape=[
            jax.ShapeDtypeStruct((n_sp, n_tp, rows, features), BF16),
            jax.ShapeDtypeStruct((n_fs * depth, 5 * width), BF16),
            jax.ShapeDtypeStruct((n_sp,) + offsets.shape, F32),
            jax.ShapeDtypeStruct((n_tp * o_rows, n_fs * o_cols), BF16),
            jax.ShapeDtypeStruct((n_tp,) + conv_gain.shape, F32),
        ],
        in_specs=[ANY] * 9,
        out_specs=[ANY] * 5,
        scratch_shapes=[
            pltpu.VMEM((depth, 5 * width), BF16),
            dma((n_sp - 1,)), dma((n_sp - 1,)), dma((n_sp - 1,)), dma((n_sp - 1,)),
            dma((n_sp,)), dma((n_sp,)),
            dma((6,)), dma((6,)),
            dma((n_sp - 1,)), dma((n_sp - 1,)),
            dma((9,)),
        ] + OUT_SEMS + [dma((2,))],
        compiler_params=pltpu.CompilerParams(collective_id=0, has_side_effects=True),
        name="gather_inputs",
    )(tokens, *w_ins, offsets, w_out, conv_gain)


def compute_body(n_sp, n_tp, width, heads, taps, blk, *refs):
    tok, gain, w, off, ck, cgain, wa_hbm, wc_own, mixed = refs[:9]
    attn_out, conv_out, mean_out, proj, gated, wa, wc, x_all, mean_all, send, recv, loc, wa_sem = refs[9:22]
    length, n_rows = tok.shape[0], mean_out.shape[2]
    gather = OutGather(wc_own, wc, refs[22:])
    z, tp, fs = lax.axis_index("sp"), lax.axis_index("tp"), lax.axis_index("fs")
    xn, yn, _ = plane(fs)
    me, place, n = z * n_tp + tp, tp * n_sp + z, n_sp * n_tp
    fetch = pltpu.make_async_copy(wa_hbm, wa, wa_sem.at[0])
    fetch.start()
    peers = [(me + d) % n for d in range(1, n)]
    greet([{"sp": p // n_tp, "tp": p % n_tp} for p in peers] + [{"fs": xn}, {"fs": yn}])
    gather.start()

    def pair(k, dest, slot):
        at = pl.ds(pl.multiple_of(dest * n_rows, n_rows), n_rows)
        if k == 2:
            return mean_out.at[dest], mean_all.at[slot]
        there = pl.ds(pl.multiple_of((k * n + slot) * width, width), width)
        return (attn_out, conv_out)[k].at[at], x_all.at[:, there]

    def ship(k, sp, core):
        src, dst = pair(k, sp * n_tp + core, place)
        mine = jnp.logical_and(z == sp, tp == core)

        @pl.when(mine)
        def _():
            pltpu.make_async_copy(src, dst, loc.at[k]).start()

        @pl.when(jnp.logical_not(mine))
        def _():
            remote(src, dst, send.at[k, sp * n_tp + core], recv.at[k, place], sp=sp, tp=core).start()

    def project(i, _):
        at = pl.ds(pl.multiple_of(i * 128, 128), 128)
        x = tok[at, :].astype(F32)
        normed = (x * lax.rsqrt(jnp.mean(x * x, axis=1, keepdims=True) + 1e-06) * gain[...]).astype(BF16)
        out = jnp.dot(normed, w[...], preferred_element_type=F32).astype(BF16)
        proj[at, :] = out[:, : 3 * width]
        value = out[:, 3 * width : 4 * width].astype(F32)
        gate = out[:, 4 * width :].astype(F32)
        gated[pl.ds(pl.multiple_of(i * 128 + 32, 32), 128), :] = (value * jax.nn.sigmoid(gate)).astype(BF16).astype(F32)
        return 0

    gated[pl.ds(0, 32), :] = jnp.zeros((32, width), F32)
    lax.fori_loop(0, length // 128, project, 0)

    ones = jnp.full((8, width), 1.0 / width, F32)

    def convolve(i, _):
        base = pl.multiple_of(i * n_rows, n_rows)
        window = gated[pl.ds(base, n_rows + 32), :]
        total = jnp.zeros((n_rows, width), F32)
        for tap in range(taps):
            lo = 32 - (taps - 1) + tap
            total = total + ck[tap : tap + 1, :] * window[lo : lo + n_rows]
        local = jnp.mean(total, axis=1, keepdims=True)
        conv_out[pl.ds(base, n_rows), :] = (total - local).astype(BF16)
        mean_out[i] = lax.dot_general(
            ones, total, (((1,), (1,)), ((), ())), precision=lax.Precision.HIGHEST, preferred_element_type=F32
        )
        return 0

    lax.fori_loop(0, length // n_rows, convolve, 0)

    row = lax.broadcasted_iota(jnp.int32, (blk, blk), 0)
    col = lax.broadcasted_iota(jnp.int32, (blk, blk), 1)
    allowed = col < row
    after = jnp.where(row >= col, 1.0, 0.0).astype(BF16)
    lane = lax.broadcasted_iota(jnp.int32, (blk, width), 1)

    def attend(i):
        q_at = pl.ds(i * blk, blk)
        mine = [jnp.logical_and(lane >= h * HD, lane < (h + 1) * HD) for h in range(heads)]
        q_all = proj[q_at, :width].astype(F32) * HD ** (-0.5)
        qs = [jnp.where(m, q_all, 0.0).astype(BF16) for m in mine]

        def pieces(j, state, diagonal):
            k_at = pl.ds(pl.multiple_of(j * blk, blk), blk)
            k = proj[k_at, width : 2 * width]
            v = proj[k_at, 2 * width : 3 * width]
            result = []
            for h, (carry, total) in enumerate(state):
                s = lax.dot_general(qs[h], k, (((1,), (1,)), ((), ())), preferred_element_type=F32)
                s = s + off[j, h : h + 1, :]
                keep = jnp.minimum(-s, 0.0) - jnp.log(1.0 + jnp.exp(-jnp.abs(s)))
                if diagonal:
                    keep = jnp.where(allowed, keep, 0.0)
                high = keep.astype(BF16)
                low = (keep - high.astype(F32)).astype(BF16)
                suffix = jnp.dot(high, after, preferred_element_type=F32)
                suffix = suffix + jnp.dot(low, after, preferred_element_type=F32)
                weights = jnp.exp(s + suffix + carry)
                if diagonal:
                    weights = jnp.where(allowed, weights, 0.0)
                total = total + jnp.dot(weights.astype(BF16), v, preferred_element_type=F32)
                result.append((carry + suffix[:, :1], total))
            return tuple(result)

        state = tuple((jnp.zeros((blk, 1), F32), jnp.zeros((blk, width), F32)) for _ in range(heads))
        state = pieces(i, state, True)
        if i:
            state = lax.fori_loop(0, i, lambda t, c: pieces(i - 1 - t, c, False), state)
        merged = state[0][1]
        for h in range(1, heads):
            merged = jnp.where(mine[h], state[h][1], merged)
        attn_out[q_at, :] = merged.astype(BF16)

    for step, i in enumerate(reversed(range(n_sp))):
        attend(i)
        if step == 0:
            for sp in range(n_sp):
                for core in range(n_tp):
                    ship(1, sp, core)
                    ship(2, sp, core)
        else:
            for core in range(n_tp):
                ship(0, i + 1, core)
        if step == (n_sp - 1) // 2:
            gather.middle()
    gather.finish()
    for core in range(n_tp):
        ship(0, 0, core)
    fetch.wait()

    def arrive(k):
        src, dst = pair(k, me, place)
        pltpu.make_async_copy(src, dst, loc.at[k]).wait()
        for d in range(1, n):
            source = (me - d + n) % n
            slot = (source % n_tp) * n_sp + source // n_tp
            src, dst = pair(k, me, slot)
            remote(src, dst, send.at[k, me], recv.at[k, slot], tp=1 - tp).wait_recv()

    arrive(2)
    arrive(1)
    square = (lax.broadcasted_iota(jnp.int32, (n_rows, n_rows), 0)
              == lax.broadcasted_iota(jnp.int32, (n_rows, n_rows), 1)).astype(F32)
    local = [
        lax.dot_general(square, mean_all[g], (((1,), (1,)), ((), ())),
                        precision=lax.Precision.HIGHEST, preferred_element_type=F32)[:, :1]
        for g in range(n)
    ]
    mean = sum(local) / n
    base = n * width
    centred = [
        x_all[:, base + g * width : base + (g + 1) * width].astype(F32) + (local[g] - mean) for g in range(n)
    ]
    shift = sum(jnp.sum(c, axis=1, keepdims=True) for c in centred) / base
    centred = [c - shift for c in centred]
    spread = sum(jnp.sum(c * c, axis=1, keepdims=True) for c in centred) / base
    scale = lax.rsqrt(spread + 1e-06)
    hidden = []
    for g, c in enumerate(centred):
        y = c * scale * cgain[:, g * width : (g + 1) * width]
        hidden.append((y * jax.nn.sigmoid(y)).astype(BF16))
    hidden = jnp.concatenate(hidden, axis=1)
    arrive(0)
    chunk = wc_own.shape[1]

    def output(c, _):
        at = pl.ds(pl.multiple_of(c * chunk, chunk), chunk)
        total = jnp.dot(x_all[:, :base], wa[:, at], preferred_element_type=F32)
        total = total + jnp.dot(hidden, wc[:, at], preferred_element_type=F32)
        mixed[:, at] = total.astype(BF16)
        return 0

    lax.fori_loop(0, wc.shape[1] // chunk, output, 0)
    for d in range(1, n):
        p = (me + d) % n
        for k in range(3):
            src, dst = pair(k, p, place)
            remote(src, dst, send.at[k, p], recv.at[k, place], tp=1 - tp).wait_send()


def compute_call(n_sp, n_tp, width, heads, blk, tok, gain, w, off, ck, cgain, wa, w_out):
    length = tok.shape[0]
    n = n_sp * n_tp
    rows = length // n
    dma = pltpu.SemaphoreType.DMA
    return pl.pallas_call(
        functools.partial(compute_body, n_sp, n_tp, width, heads, ck.shape[0], blk),
        out_shape=jax.ShapeDtypeStruct((rows, wa.shape[1]), BF16),
        in_specs=[VMEM] * 6 + [ANY] * 2,
        out_specs=VMEM,
        scratch_shapes=[
            pltpu.VMEM((length, width), BF16),
            pltpu.VMEM((length, width), BF16),
            pltpu.VMEM((n, 8, rows), F32),
            pltpu.VMEM((length, 3 * width), BF16),
            pltpu.VMEM((length + 32, width), F32),
            pltpu.VMEM(wa.shape, BF16),
            pltpu.VMEM(wa.shape, BF16),
            pltpu.VMEM((rows, 2 * n * width), BF16),
            pltpu.VMEM((n, 8, rows), F32),
            dma((3, n)), dma((3, n)), dma((3,)), dma((1,)),
        ] + OUT_SEMS,
        compiler_params=pltpu.CompilerParams(collective_id=1, has_side_effects=True),
        name="branches",
    )(tok, gain, w, off, ck, cgain, wa, w_out)


def spread_shards(
    tokens,
    norm_gain,
    w_query,
    w_key,
    w_value,
    w_conv_value,
    w_conv_gate,
    key_offset,
    conv_kernel,
    conv_gain,
    w_attn_out,
    w_conv_out,
):
    n_sp, n_fs, n_tp = (lax.axis_size(a) for a in ("sp", "fs", "tp"))
    z = lax.axis_index("sp")
    width = w_query.shape[1] // n_sp
    heads = width // HD
    offsets = jnp.transpose(key_offset.astype(F32))
    tok_all, w_all, off_all, wa, cgain = gather_call(
        n_sp, n_fs, n_tp, width, tokens[0],
        (w_query, w_key, w_value, w_conv_value, w_conv_gate), offsets, w_attn_out, conv_gain[None],
    )
    tok_all = tok_all.reshape(-1, tokens.shape[2])
    off = lax.dynamic_slice_in_dim(off_all, z * heads, heads, axis=1)
    taps = lax.dynamic_slice_in_dim(conv_kernel, z * width, width, axis=1)
    mixed = compute_call(
        n_sp, n_tp, width, heads, key_offset.shape[0], tok_all, norm_gain[None], w_all, off, taps,
        cgain.reshape(1, -1), wa, w_conv_out,
    )
    return mixed[None]


def shifted(block, axis, distance):
    devices = range(lax.axis_size(axis))
    route = [(i - distance, i) for i in devices if i - distance in devices]
    return lax.ppermute(block, axis, route)


def piece_terms(queries, key_rows, value_rows, offsets, carry_log, allowed):
    head_size = queries.shape[2]
    logits = jnp.einsum(
        "qhd,khd->hqk", queries, key_rows, preferred_element_type=jnp.float32
    ) * head_size ** (-0.5)
    logits = logits + jnp.transpose(offsets.astype(jnp.float32))[:, None, :]
    log_keep = jax.nn.log_sigmoid(-logits)
    if allowed is not None:
        log_keep = jnp.where(allowed[None], log_keep, 0.0)
    between = lax.cumsum(log_keep, axis=2, reverse=True) - log_keep
    weights = jnp.exp(jax.nn.log_sigmoid(logits) + between + carry_log[:, :, None])
    if allowed is not None:
        weights = jnp.where(allowed[None], weights, 0.0)
    result = jnp.einsum(
        "hqk,khd->qhd", weights.astype(jnp.bfloat16), value_rows, preferred_element_type=jnp.float32
    )
    return (result, carry_log + jnp.sum(log_keep, axis=2))


def shards(
    tokens,
    norm_gain,
    w_query,
    w_key,
    w_value,
    w_conv_value,
    w_conv_gate,
    key_offset,
    conv_kernel,
    conv_gain,
    w_attn_out,
    w_conv_out,
):
    gathered = (
        lax.all_gather(w_query, "fs", axis=0, tiled=True),
        lax.all_gather(w_key, "fs", axis=0, tiled=True),
        lax.all_gather(w_value, "fs", axis=0, tiled=True),
        lax.all_gather(w_conv_value, "fs", axis=0, tiled=True),
        lax.all_gather(w_conv_gate, "fs", axis=0, tiled=True),
    )
    floats = lax.all_gather(tokens[0], "tp", axis=0, tiled=True).astype(jnp.float32)
    normed = (
        floats * lax.rsqrt(jnp.mean(floats * floats, axis=1, keepdims=True) + 1e-06) * norm_gain
    ).astype(jnp.bfloat16)
    projected = jnp.concatenate(
        [
            jnp.dot(normed, weight, preferred_element_type=jnp.float32).astype(jnp.bfloat16)
            for weight in gathered
        ],
        axis=1,
    )
    head_cols = w_query.shape[1]
    channels = w_conv_value.shape[1]
    block_len = projected.shape[0]
    local_heads = head_cols // HD
    queries = projected[:, :head_cols].reshape(block_len, local_heads, HD)
    key_flat = projected[:, head_cols : 2 * head_cols]
    value_flat = projected[:, 2 * head_cols : 3 * head_cols]
    conv_value = projected[:, 3 * head_cols : 3 * head_cols + channels]
    conv_gate = projected[:, 3 * head_cols + channels :]
    position = lax.axis_index("sp")
    positions = jnp.arange(block_len, dtype=jnp.int32)
    causal = positions[None, :] < positions[:, None]
    start_log = jnp.zeros((local_heads, block_len), jnp.float32)
    totals, carry_log = piece_terms(
        queries,
        key_flat.reshape(block_len, local_heads, HD),
        value_flat.reshape(block_len, local_heads, HD),
        key_offset,
        start_log,
        causal,
    )

    def visit(hop_count, carried):
        running, running_log, moving = carried
        moving = shifted((moving[0], moving[1], moving[2]), "sp", 1)
        result, next_log = piece_terms(
            queries,
            moving[0].reshape(block_len, local_heads, HD),
            moving[1].reshape(block_len, local_heads, HD),
            moving[2],
            running_log,
            None,
        )
        active = position >= hop_count
        running = jnp.where(active, running + result, running)
        running_log = jnp.where(active, next_log, running_log)
        return (running, running_log, moving)

    totals, carry_log, leftover = lax.fori_loop(
        1, lax.axis_size("sp"), visit, (totals, carry_log, (key_flat, value_flat, key_offset))
    )
    attn_heads = totals.reshape(block_len, head_cols).astype(jnp.bfloat16)
    gated_input = (
        conv_value.astype(jnp.float32) * jax.nn.sigmoid(conv_gate.astype(jnp.float32))
    ).astype(jnp.bfloat16)
    kernel_len = conv_kernel.shape[0]
    edge_rows = shifted(gated_input[block_len - (kernel_len - 1) :], "sp", 1)
    extended = jnp.concatenate([edge_rows, gated_input], axis=0).astype(jnp.float32)
    conv_sum = jnp.zeros((block_len, channels), jnp.float32)
    for tap_index in range(kernel_len):
        conv_sum = conv_sum + conv_kernel[tap_index] * extended[tap_index : tap_index + block_len]
    channel_total = lax.psum(jnp.sum(conv_sum, axis=1), "tp")
    centred = conv_sum - (channel_total / CC)[:, None]
    spread = lax.psum(jnp.sum(centred * centred, axis=1), "tp") / CC
    conv_hidden = jax.nn.silu(centred * lax.rsqrt(spread + 1e-06)[:, None] * conv_gain).astype(
        jnp.bfloat16
    )
    attn_weight, conv_weight = (
        lax.all_gather(w_attn_out, "fs", axis=1, tiled=True),
        lax.all_gather(w_conv_out, "fs", axis=1, tiled=True),
    )
    partial_value = jnp.dot(attn_heads, attn_weight, preferred_element_type=jnp.float32)
    partial_value = partial_value + jnp.dot(
        conv_hidden, conv_weight, preferred_element_type=jnp.float32
    )
    mixed = lax.psum_scatter(
        lax.optimization_barrier(partial_value.astype(jnp.bfloat16))
        .astype(jnp.float32)
        .astype(jnp.bfloat16),
        "tp",
        scatter_dimension=0,
        tiled=True,
    )
    return mixed[None]


def solution(mesh):
    placed = (
        P("fs", ("sp", "tp"), None),
        P(),
        P("fs", "tp"),
        P("fs", "tp"),
        P("fs", "tp"),
        P("fs", "tp"),
        P("fs", "tp"),
        P("sp", "tp"),
        P(None, "tp"),
        P("tp"),
        P("tp", "fs"),
        P("tp", "fs"),
    )

    def fits(tokens, norm_gain, w_query, *rest):
        n_sp, n_fs, n_tp = mesh.shape["sp"], mesh.shape["fs"], mesh.shape["tp"]
        cols = w_query.shape[1] // n_tp
        return n_fs == 4 and n_tp == 2 and n_sp > 1 and rest[5].shape[0] <= 33 and cols % (128 * n_sp) == 0 and rest[2].shape[1] == w_query.shape[1] and (
            tokens.shape[1] % (128 * n_sp * n_tp) == 0
        )

    def program(*args):
        body = spread_shards if fits(*args) else shards
        return mapped(body)(*args)

    def mapped(body):
        return jax.shard_map(
            body, mesh=mesh, in_specs=placed, out_specs=P("fs", ("sp", "tp"), None), check_vma=False
        )

    return program
```

```python
import functools

import jax
import jax.numpy as jnp
from jax import lax
from jax.experimental import pallas as pl
from jax.experimental.pallas import tpu as pltpu
from jax.sharding import PartitionSpec as P

HD = 64
CC = 1024
MESH = pl.DeviceIdType.MESH
F32 = jnp.float32
BF16 = jnp.bfloat16


def remote(src, dst, send, recv, **where):
    return pltpu.make_async_remote_copy(
        src_ref=src, dst_ref=dst, send_sem=send, recv_sem=recv, device_id=where, device_id_type=MESH
    )


def greet(peers):
    barrier = pltpu.get_barrier_semaphore()
    for where in peers:
        pl.semaphore_signal(barrier, inc=1, device_id=where, device_id_type=MESH)
    pl.semaphore_wait(barrier, len(peers))


def plane(fs):
    y = (fs + 2) % 4
    return fs + 1 - 2 * (fs % 2), y, y + 1 - 2 * (y % 2)


class OutGather:
    def __init__(self, source, target, sems):
        half = source.shape[0] // 2
        self.sources = [source.at[pl.ds(k * half, half)] for k in range(2)]
        self.target = target
        self.send, self.recv, self.psend, self.precv, self.local = sems
        self.fs, self.tp = lax.axis_index("fs"), lax.axis_index("tp")

    def slot(self, k, owner, group):
        rows, cols = self.sources[k].shape
        return self.target.at[
            pl.ds(pl.multiple_of((group * 2 + k) * rows, rows), rows),
            pl.ds(pl.multiple_of(owner * cols, cols), cols),
        ]

    def hop(self, src, k, owner, sem, to):
        return remote(src, self.slot(k, owner, self.tp), self.send.at[sem], self.recv.at[sem], fs=to)

    def other(self, src, k, owner, sem):
        return remote(
            src, self.slot(k, owner, self.tp), self.psend.at[sem], self.precv.at[sem], tp=1 - self.tp
        )

    def plan(self):
        fs = self.fs
        xn, yn, dg = plane(fs)
        a, c = self.sources
        self.first = [
            self.hop(a, 0, fs, 0, xn), self.hop(c, 1, fs, 1, yn),
            self.hop(c, 1, fs, 2, xn), self.hop(a, 0, fs, 3, yn),
        ]
        self.relay = [
            self.hop(self.slot(0, xn, self.tp), 0, xn, 4, yn),
            self.hop(self.slot(1, yn, self.tp), 1, yn, 5, xn),
        ]
        arrivals = [(0, 0, xn), (1, 1, yn), (2, 1, xn), (3, 0, yn), (4, 0, dg), (5, 1, dg)]
        self.got = [
            (self.hop(self.slot(k, o, self.tp), k, o, s, xn), self.other(self.slot(k, o, self.tp), k, o, s))
            for s, k, o in arrivals
        ]
        self.own = [self.other(a, 0, fs, 6), self.other(c, 1, fs, 7)]
        self.keep = [
            pltpu.make_async_copy(self.sources[k], self.slot(k, fs, self.tp), self.local.at[k]) for k in (0, 1)
        ]

    def start(self):
        self.plan()
        for copy in self.first + self.own + self.keep:
            copy.start()

    def middle(self):
        for s in range(4):
            arrived, onward = self.got[s]
            arrived.wait_recv()
            if s < 2:
                self.relay[s].start()
            onward.start()

    def finish(self):
        for s in (4, 5):
            arrived, onward = self.got[s]
            arrived.wait_recv()
            onward.start()
        for copy in self.first + self.relay:
            copy.wait_send()
        for _, onward in self.got:
            onward.wait()
        for copy in self.own:
            copy.wait()
        for copy in self.keep:
            copy.wait()


OUT_SEMS = [
    pltpu.SemaphoreType.DMA((6,)),
    pltpu.SemaphoreType.DMA((6,)),
    pltpu.SemaphoreType.DMA((8,)),
    pltpu.SemaphoreType.DMA((8,)),
    pltpu.SemaphoreType.DMA((2,)),
]


def gather_kernel(n_sp, with_out, *refs):
    tok, w_ins, off = refs[0], refs[1:6], refs[6]
    refs = refs[7:]
    if with_out:
        out_source, cgain, refs = refs[0], refs[1], refs[2:]
    tok_all, w_all, off_all = refs[:3]
    refs = refs[3:]
    if with_out:
        out_target, cgain_all, refs = refs[0], refs[1], refs[2:]
    stage, up_s, up_r, dn_s, dn_r, par_s, par_r, w_s, w_r, off_s, off_r, loc = refs[:12]
    z, fs, tp = lax.axis_index("sp"), lax.axis_index("fs"), lax.axis_index("tp")
    xn, yn, dg = plane(fs)
    rows = w_ins[0].shape[0]
    width = stage.shape[1] // 5
    half = rows // 2

    fills = [
        pltpu.make_async_copy(
            w.at[:, pl.ds(pl.multiple_of(z * width, width), width)],
            stage.at[:, pl.ds(k * width, width)],
            loc.at[k],
        )
        for k, w in enumerate(w_ins)
    ]
    for fill in fills:
        fill.start()
    keep_tok = pltpu.make_async_copy(tok, tok_all.at[z, tp], loc.at[5])
    keep_off = pltpu.make_async_copy(off, off_all.at[z], loc.at[6])
    keep_gain = pltpu.make_async_copy(cgain, cgain_all.at[tp], loc.at[8])
    keep_tok.start()
    keep_off.start()
    keep_gain.start()
    greet(
        [{"sp": (z + d) % n_sp} for d in range(1, n_sp)]
        + [{"fs": xn}, {"fs": yn}, {"tp": 1 - tp}]
    )

    def lift(src, block, dist):
        return remote(src, tok_all.at[block, tp], up_s.at[dist - 1], up_r.at[dist - 1], sp=(z + 1) % n_sp)

    def sink(src, block, dist):
        return remote(src, tok_all.at[block, tp], dn_s.at[dist - 1], dn_r.at[dist - 1], sp=(z + n_sp - 1) % n_sp)

    def across(src, block):
        return remote(src, tok_all.at[block, tp], par_s.at[block], par_r.at[block], tp=1 - tp)

    @pl.when(z < n_sp - 1)
    def _():
        lift(tok, z, 1).start()

    @pl.when(z > 0)
    def _():
        sink(tok, z, 1).start()

    across(tok, z).start()
    offs = [
        remote(off, off_all.at[z], off_s.at[d - 1], off_r.at[d - 1], sp=(z + d) % n_sp) for d in range(1, n_sp)
    ]
    gain_copy = remote(cgain, cgain_all.at[tp], refs[17].at[0], refs[17].at[1], tp=1 - tp)
    gain_copy.start()
    for copy in offs:
        copy.start()
    for fill in fills:
        fill.wait()
    keep_w = pltpu.make_async_copy(stage, w_all.at[pl.ds(pl.multiple_of(fs * rows, rows), rows)], loc.at[7])
    keep_w.start()

    def part(owner, h):
        return w_all.at[pl.ds(pl.multiple_of(owner * rows + h * half, half), half)]

    def send_w(src, owner, h, sem, to):
        return remote(src, part(owner, h), w_s.at[sem], w_r.at[sem], fs=to)

    own = [stage.at[pl.ds(h * half, half)] for h in range(2)]
    first = [
        send_w(own[0], fs, 0, 0, xn), send_w(own[1], fs, 1, 1, yn),
        send_w(own[1], fs, 1, 2, xn), send_w(own[0], fs, 0, 3, yn),
    ]
    for copy in first:
        copy.start()
    relay = [send_w(part(xn, 0), xn, 0, 4, yn), send_w(part(yn, 1), yn, 1, 5, xn)]
    if with_out:
        gather = OutGather(out_source, out_target, refs[12:17])
    arrivals = [(0, xn, 0), (1, yn, 1), (2, xn, 1), (3, yn, 0), (4, dg, 0), (5, dg, 1)]
    for s, owner, h in arrivals[:2]:
        send_w(part(owner, h), owner, h, s, xn).wait_recv()
        relay[s].start()
    if with_out:
        gather.start()

    for dist in range(1, n_sp):
        if with_out and dist == n_sp - 1:
            gather.middle()

        @pl.when(z >= dist)
        def _():
            block = (z - dist + n_sp) % n_sp
            lift(tok_all.at[block, tp], block, dist).wait_recv()
            if dist < n_sp - 1:
                @pl.when(z < n_sp - 1)
                def _():
                    lift(tok_all.at[block, tp], block, dist + 1).start()
            across(tok_all.at[block, tp], block).start()

        @pl.when(z + dist < n_sp)
        def _():
            block = (z + dist) % n_sp
            sink(tok_all.at[block, tp], block, dist).wait_recv()
            if dist < n_sp - 1:
                @pl.when(z > 0)
                def _():
                    sink(tok_all.at[block, tp], block, dist + 1).start()
            across(tok_all.at[block, tp], block).start()

    for s, owner, h in arrivals[2:]:
        send_w(part(owner, h), owner, h, s, xn).wait_recv()
    if with_out:
        gather.finish()
    for copy in first + relay:
        copy.wait_send()
    for dist in range(1, n_sp):
        @pl.when(jnp.logical_and(z < n_sp - 1, z >= dist - 1))
        def _():
            lift(tok, z, dist).wait_send()

        @pl.when(jnp.logical_and(z > 0, z + dist - 1 < n_sp))
        def _():
            sink(tok, z, dist).wait_send()

    for block in range(n_sp):
        remote(tok, tok_all.at[block, 1 - tp], par_s.at[block], par_r.at[block], tp=1 - tp).wait()
    for copy in offs:
        copy.wait()
    gain_copy.wait()
    keep_gain.wait()
    keep_tok.wait()
    keep_off.wait()
    keep_w.wait()


ANY = pl.BlockSpec(memory_space=pl.ANY)
VMEM = pl.BlockSpec(memory_space=pltpu.VMEM)


def gather_call(n_sp, n_fs, n_tp, width, tokens, w_ins, offsets, w_out, conv_gain):
    rows, features = tokens.shape
    depth = w_ins[0].shape[0]
    o_rows, o_cols = w_out.shape
    dma = pltpu.SemaphoreType.DMA
    return pl.pallas_call(
        functools.partial(gather_kernel, n_sp, True),
        out_shape=[
            jax.ShapeDtypeStruct((n_sp, n_tp, rows, features), BF16),
            jax.ShapeDtypeStruct((n_fs * depth, 5 * width), BF16),
            jax.ShapeDtypeStruct((n_sp,) + offsets.shape, F32),
            jax.ShapeDtypeStruct((n_tp * o_rows, n_fs * o_cols), BF16),
            jax.ShapeDtypeStruct((n_tp,) + conv_gain.shape, F32),
        ],
        in_specs=[ANY] * 9,
        out_specs=[ANY] * 5,
        scratch_shapes=[
            pltpu.VMEM((depth, 5 * width), BF16),
            dma((n_sp - 1,)), dma((n_sp - 1,)), dma((n_sp - 1,)), dma((n_sp - 1,)),
            dma((n_sp,)), dma((n_sp,)),
            dma((6,)), dma((6,)),
            dma((n_sp - 1,)), dma((n_sp - 1,)),
            dma((9,)),
        ] + OUT_SEMS + [dma((2,))],
        compiler_params=pltpu.CompilerParams(collective_id=0, has_side_effects=True),
        name="gather_inputs",
    )(tokens, *w_ins, offsets, w_out, conv_gain)


def compute_body(n_sp, n_tp, width, heads, taps, blk, *refs):
    tok_hbm, gain, w_hbm, off, ck, cgain, wa_hbm, wc_own, mixed = refs[:9]
    attn_out, conv_out, mean_out, proj, gated, wa, wc, x_all, mean_all, send, recv, loc, wa_sem, tok, w, tok_sem = refs[9:25]
    length, n_rows = tok.shape[0], mean_out.shape[2]
    gather = OutGather(wc_own, wc, refs[25:])
    z, tp, fs = lax.axis_index("sp"), lax.axis_index("tp"), lax.axis_index("fs")
    xn, yn, _ = plane(fs)
    me, place, n = z * n_tp + tp, tp * n_sp + z, n_sp * n_tp
    fetch = pltpu.make_async_copy(wa_hbm, wa, wa_sem.at[0])
    load_w = pltpu.make_async_copy(w_hbm, w, wa_sem.at[1])

    def load(i):
        at = pl.ds(pl.multiple_of(i * 128, 128), 128)
        return pltpu.make_async_copy(tok_hbm.at[at], tok.at[at], tok_sem.at[i])

    load_w.start()
    for i in range(length // 128):
        load(i).start()
    fetch.start()
    peers = [(me + d) % n for d in range(1, n)]
    greet([{"sp": p // n_tp, "tp": p % n_tp} for p in peers] + [{"fs": xn}, {"fs": yn}])
    gather.start()

    def pair(k, dest, slot):
        at = pl.ds(pl.multiple_of(dest * n_rows, n_rows), n_rows)
        if k == 2:
            return mean_out.at[dest], mean_all.at[slot]
        there = pl.ds(pl.multiple_of((k * n + slot) * width, width), width)
        return (attn_out, conv_out)[k].at[at], x_all.at[:, there]

    def ship(k, sp, core):
        src, dst = pair(k, sp * n_tp + core, place)
        mine = jnp.logical_and(z == sp, tp == core)

        @pl.when(mine)
        def _():
            pltpu.make_async_copy(src, dst, loc.at[k]).start()

        @pl.when(jnp.logical_not(mine))
        def _():
            remote(src, dst, send.at[k, sp * n_tp + core], recv.at[k, place], sp=sp, tp=core).start()

    def project(i, _):
        at = pl.ds(pl.multiple_of(i * 128, 128), 128)
        load(i).wait()
        x = tok[at, :].astype(F32)
        normed = (x * lax.rsqrt(jnp.mean(x * x, axis=1, keepdims=True) + 1e-06) * gain[...]).astype(BF16)
        out = jnp.dot(normed, w[...], preferred_element_type=F32).astype(BF16)
        proj[at, :] = out[:, : 3 * width]
        value = out[:, 3 * width : 4 * width].astype(F32)
        gate = out[:, 4 * width :].astype(F32)
        gated[pl.ds(pl.multiple_of(i * 128 + 32, 32), 128), :] = (value * jax.nn.sigmoid(gate)).astype(BF16).astype(F32)
        return 0

    gated[pl.ds(0, 32), :] = jnp.zeros((32, width), F32)
    load_w.wait()
    lax.fori_loop(0, length // 128, project, 0)

    ones = jnp.full((8, width), 1.0 / width, F32)

    def convolve(i, _):
        base = pl.multiple_of(i * n_rows, n_rows)
        window = gated[pl.ds(base, n_rows + 32), :]
        total = jnp.zeros((n_rows, width), F32)
        for tap in range(taps):
            lo = 32 - (taps - 1) + tap
            total = total + ck[tap : tap + 1, pl.ds(pl.multiple_of(z * width, width), width)] * window[lo : lo + n_rows]
        local = jnp.mean(total, axis=1, keepdims=True)
        conv_out[pl.ds(base, n_rows), :] = (total - local).astype(BF16)
        mean_out[i] = lax.dot_general(
            ones, total, (((1,), (1,)), ((), ())), precision=lax.Precision.HIGHEST, preferred_element_type=F32
        )
        return 0

    lax.fori_loop(0, length // n_rows, convolve, 0)

    row = lax.broadcasted_iota(jnp.int32, (blk, blk), 0)
    col = lax.broadcasted_iota(jnp.int32, (blk, blk), 1)
    allowed = col < row
    after = jnp.where(row >= col, 1.0, 0.0).astype(BF16)
    lane = lax.broadcasted_iota(jnp.int32, (blk, width), 1)

    def attend(i):
        q_at = pl.ds(i * blk, blk)
        mine = [jnp.logical_and(lane >= h * HD, lane < (h + 1) * HD) for h in range(heads)]
        q_all = proj[q_at, :width].astype(F32) * HD ** (-0.5)
        qs = [jnp.where(m, q_all, 0.0).astype(BF16) for m in mine]

        def pieces(j, state, diagonal):
            k_at = pl.ds(pl.multiple_of(j * blk, blk), blk)
            k = proj[k_at, width : 2 * width]
            v = proj[k_at, 2 * width : 3 * width]
            result = []
            for h, (carry, total) in enumerate(state):
                s = lax.dot_general(qs[h], k, (((1,), (1,)), ((), ())), preferred_element_type=F32)
                s = s + off[j, pl.ds(z * heads + h, 1), :]
                keep = jnp.minimum(-s, 0.0) - jnp.log(1.0 + jnp.exp(-jnp.abs(s)))
                if diagonal:
                    keep = jnp.where(allowed, keep, 0.0)
                high = keep.astype(BF16)
                low = (keep - high.astype(F32)).astype(BF16)
                suffix = jnp.dot(high, after, preferred_element_type=F32)
                suffix = suffix + jnp.dot(low, after, preferred_element_type=F32)
                weights = jnp.exp(s + suffix + carry)
                if diagonal:
                    weights = jnp.where(allowed, weights, 0.0)
                total = total + jnp.dot(weights.astype(BF16), v, preferred_element_type=F32)
                result.append((carry + suffix[:, :1], total))
            return tuple(result)

        state = tuple((jnp.zeros((blk, 1), F32), jnp.zeros((blk, width), F32)) for _ in range(heads))
        state = pieces(i, state, True)
        if i:
            state = lax.fori_loop(0, i, lambda t, c: pieces(i - 1 - t, c, False), state)
        merged = state[0][1]
        for h in range(1, heads):
            merged = jnp.where(mine[h], state[h][1], merged)
        attn_out[q_at, :] = merged.astype(BF16)

    for step, i in enumerate(reversed(range(n_sp))):
        attend(i)
        if step == 0:
            for sp in range(n_sp):
                for core in range(n_tp):
                    ship(1, sp, core)
                    ship(2, sp, core)
        else:
            for core in range(n_tp):
                ship(0, i + 1, core)
        if step == (n_sp - 1) // 2:
            gather.middle()
    gather.finish()
    for core in range(n_tp):
        ship(0, 0, core)
    fetch.wait()

    def arrive(k):
        src, dst = pair(k, me, place)
        pltpu.make_async_copy(src, dst, loc.at[k]).wait()
        for d in range(1, n):
            source = (me - d + n) % n
            slot = (source % n_tp) * n_sp + source // n_tp
            src, dst = pair(k, me, slot)
            remote(src, dst, send.at[k, me], recv.at[k, slot], tp=1 - tp).wait_recv()

    arrive(2)
    arrive(1)
    square = (lax.broadcasted_iota(jnp.int32, (n_rows, n_rows), 0)
              == lax.broadcasted_iota(jnp.int32, (n_rows, n_rows), 1)).astype(F32)
    local = [
        lax.dot_general(square, mean_all[g], (((1,), (1,)), ((), ())),
                        precision=lax.Precision.HIGHEST, preferred_element_type=F32)[:, :1]
        for g in range(n)
    ]
    mean = sum(local) / n
    base = n * width
    centred = [
        x_all[:, base + g * width : base + (g + 1) * width].astype(F32) + (local[g] - mean) for g in range(n)
    ]
    shift = sum(jnp.sum(c, axis=1, keepdims=True) for c in centred) / base
    centred = [c - shift for c in centred]
    spread = sum(jnp.sum(c * c, axis=1, keepdims=True) for c in centred) / base
    scale = lax.rsqrt(spread + 1e-06)
    hidden = []
    for g, c in enumerate(centred):
        y = c * scale * cgain[:, g * width : (g + 1) * width]
        hidden.append((y * jax.nn.sigmoid(y)).astype(BF16))
    hidden = jnp.concatenate(hidden, axis=1)
    arrive(0)
    chunk = wc_own.shape[1]

    def output(c, _):
        at = pl.ds(pl.multiple_of(c * chunk, chunk), chunk)
        total = jnp.dot(x_all[:, :base], wa[:, at], preferred_element_type=F32)
        total = total + jnp.dot(hidden, wc[:, at], preferred_element_type=F32)
        mixed[:, at] = total.astype(BF16)
        return 0

    lax.fori_loop(0, wc.shape[1] // chunk, output, 0)
    for d in range(1, n):
        p = (me + d) % n
        for k in range(3):
            src, dst = pair(k, p, place)
            remote(src, dst, send.at[k, p], recv.at[k, place], tp=1 - tp).wait_send()


def compute_call(n_sp, n_tp, width, heads, blk, tok, gain, w, off, ck, cgain, wa, w_out):
    length = tok.shape[0]
    n = n_sp * n_tp
    rows = length // n
    dma = pltpu.SemaphoreType.DMA
    return pl.pallas_call(
        functools.partial(compute_body, n_sp, n_tp, width, heads, ck.shape[0], blk),
        out_shape=jax.ShapeDtypeStruct((rows, wa.shape[1]), BF16),
        in_specs=[ANY, VMEM, ANY] + [VMEM] * 3 + [ANY] * 2,
        out_specs=VMEM,
        scratch_shapes=[
            pltpu.VMEM((length, width), BF16),
            pltpu.VMEM((length, width), BF16),
            pltpu.VMEM((n, 8, rows), F32),
            pltpu.VMEM((length, 3 * width), BF16),
            pltpu.VMEM((length + 32, width), F32),
            pltpu.VMEM(wa.shape, BF16),
            pltpu.VMEM(wa.shape, BF16),
            pltpu.VMEM((rows, 2 * n * width), BF16),
            pltpu.VMEM((n, 8, rows), F32),
            dma((3, n)), dma((3, n)), dma((3,)), dma((2,)),
            pltpu.VMEM(tok.shape, BF16),
            pltpu.VMEM(w.shape, BF16),
            dma((length // 128,)),
        ] + OUT_SEMS,
        compiler_params=pltpu.CompilerParams(collective_id=1, has_side_effects=True),
        name="branches",
    )(tok, gain, w, off, ck, cgain, wa, w_out)


def spread_shards(
    tokens,
    norm_gain,
    w_query,
    w_key,
    w_value,
    w_conv_value,
    w_conv_gate,
    key_offset,
    conv_kernel,
    conv_gain,
    w_attn_out,
    w_conv_out,
):
    n_sp, n_fs, n_tp = (lax.axis_size(a) for a in ("sp", "fs", "tp"))
    width = w_query.shape[1] // n_sp
    heads = width // HD
    offsets = jnp.transpose(key_offset.astype(F32))
    tok_all, w_all, off_all, wa, cgain = gather_call(
        n_sp, n_fs, n_tp, width, tokens[0],
        (w_query, w_key, w_value, w_conv_value, w_conv_gate), offsets, w_attn_out, conv_gain[None],
    )
    tok_all = tok_all.reshape(-1, tokens.shape[2])
    mixed = compute_call(
        n_sp, n_tp, width, heads, key_offset.shape[0], tok_all, norm_gain[None], w_all, off_all, conv_kernel,
        cgain.reshape(1, -1), wa, w_conv_out,
    )
    return mixed[None]


def shifted(block, axis, distance):
    devices = range(lax.axis_size(axis))
    route = [(i - distance, i) for i in devices if i - distance in devices]
    return lax.ppermute(block, axis, route)


def piece_terms(queries, key_rows, value_rows, offsets, carry_log, allowed):
    head_size = queries.shape[2]
    logits = jnp.einsum(
        "qhd,khd->hqk", queries, key_rows, preferred_element_type=jnp.float32
    ) * head_size ** (-0.5)
    logits = logits + jnp.transpose(offsets.astype(jnp.float32))[:, None, :]
    log_keep = jax.nn.log_sigmoid(-logits)
    if allowed is not None:
        log_keep = jnp.where(allowed[None], log_keep, 0.0)
    between = lax.cumsum(log_keep, axis=2, reverse=True) - log_keep
    weights = jnp.exp(jax.nn.log_sigmoid(logits) + between + carry_log[:, :, None])
    if allowed is not None:
        weights = jnp.where(allowed[None], weights, 0.0)
    result = jnp.einsum(
        "hqk,khd->qhd", weights.astype(jnp.bfloat16), value_rows, preferred_element_type=jnp.float32
    )
    return (result, carry_log + jnp.sum(log_keep, axis=2))


def shards(
    tokens,
    norm_gain,
    w_query,
    w_key,
    w_value,
    w_conv_value,
    w_conv_gate,
    key_offset,
    conv_kernel,
    conv_gain,
    w_attn_out,
    w_conv_out,
):
    gathered = (
        lax.all_gather(w_query, "fs", axis=0, tiled=True),
        lax.all_gather(w_key, "fs", axis=0, tiled=True),
        lax.all_gather(w_value, "fs", axis=0, tiled=True),
        lax.all_gather(w_conv_value, "fs", axis=0, tiled=True),
        lax.all_gather(w_conv_gate, "fs", axis=0, tiled=True),
    )
    floats = lax.all_gather(tokens[0], "tp", axis=0, tiled=True).astype(jnp.float32)
    normed = (
        floats * lax.rsqrt(jnp.mean(floats * floats, axis=1, keepdims=True) + 1e-06) * norm_gain
    ).astype(jnp.bfloat16)
    projected = jnp.concatenate(
        [
            jnp.dot(normed, weight, preferred_element_type=jnp.float32).astype(jnp.bfloat16)
            for weight in gathered
        ],
        axis=1,
    )
    head_cols = w_query.shape[1]
    channels = w_conv_value.shape[1]
    block_len = projected.shape[0]
    local_heads = head_cols // HD
    queries = projected[:, :head_cols].reshape(block_len, local_heads, HD)
    key_flat = projected[:, head_cols : 2 * head_cols]
    value_flat = projected[:, 2 * head_cols : 3 * head_cols]
    conv_value = projected[:, 3 * head_cols : 3 * head_cols + channels]
    conv_gate = projected[:, 3 * head_cols + channels :]
    position = lax.axis_index("sp")
    positions = jnp.arange(block_len, dtype=jnp.int32)
    causal = positions[None, :] < positions[:, None]
    start_log = jnp.zeros((local_heads, block_len), jnp.float32)
    totals, carry_log = piece_terms(
        queries,
        key_flat.reshape(block_len, local_heads, HD),
        value_flat.reshape(block_len, local_heads, HD),
        key_offset,
        start_log,
        causal,
    )

    def visit(hop_count, carried):
        running, running_log, moving = carried
        moving = shifted((moving[0], moving[1], moving[2]), "sp", 1)
        result, next_log = piece_terms(
            queries,
            moving[0].reshape(block_len, local_heads, HD),
            moving[1].reshape(block_len, local_heads, HD),
            moving[2],
            running_log,
            None,
        )
        active = position >= hop_count
        running = jnp.where(active, running + result, running)
        running_log = jnp.where(active, next_log, running_log)
        return (running, running_log, moving)

    totals, carry_log, leftover = lax.fori_loop(
        1, lax.axis_size("sp"), visit, (totals, carry_log, (key_flat, value_flat, key_offset))
    )
    attn_heads = totals.reshape(block_len, head_cols).astype(jnp.bfloat16)
    gated_input = (
        conv_value.astype(jnp.float32) * jax.nn.sigmoid(conv_gate.astype(jnp.float32))
    ).astype(jnp.bfloat16)
    kernel_len = conv_kernel.shape[0]
    edge_rows = shifted(gated_input[block_len - (kernel_len - 1) :], "sp", 1)
    extended = jnp.concatenate([edge_rows, gated_input], axis=0).astype(jnp.float32)
    conv_sum = jnp.zeros((block_len, channels), jnp.float32)
    for tap_index in range(kernel_len):
        conv_sum = conv_sum + conv_kernel[tap_index] * extended[tap_index : tap_index + block_len]
    channel_total = lax.psum(jnp.sum(conv_sum, axis=1), "tp")
    centred = conv_sum - (channel_total / CC)[:, None]
    spread = lax.psum(jnp.sum(centred * centred, axis=1), "tp") / CC
    conv_hidden = jax.nn.silu(centred * lax.rsqrt(spread + 1e-06)[:, None] * conv_gain).astype(
        jnp.bfloat16
    )
    attn_weight, conv_weight = (
        lax.all_gather(w_attn_out, "fs", axis=1, tiled=True),
        lax.all_gather(w_conv_out, "fs", axis=1, tiled=True),
    )
    partial_value = jnp.dot(attn_heads, attn_weight, preferred_element_type=jnp.float32)
    partial_value = partial_value + jnp.dot(
        conv_hidden, conv_weight, preferred_element_type=jnp.float32
    )
    mixed = lax.psum_scatter(
        lax.optimization_barrier(partial_value.astype(jnp.bfloat16))
        .astype(jnp.float32)
        .astype(jnp.bfloat16),
        "tp",
        scatter_dimension=0,
        tiled=True,
    )
    return mixed[None]


def solution(mesh):
    placed = (
        P("fs", ("sp", "tp"), None),
        P(),
        P("fs", "tp"),
        P("fs", "tp"),
        P("fs", "tp"),
        P("fs", "tp"),
        P("fs", "tp"),
        P("sp", "tp"),
        P(None, "tp"),
        P("tp"),
        P("tp", "fs"),
        P("tp", "fs"),
    )

    def fits(tokens, norm_gain, w_query, *rest):
        n_sp, n_fs, n_tp = mesh.shape["sp"], mesh.shape["fs"], mesh.shape["tp"]
        cols = w_query.shape[1] // n_tp
        return n_fs == 4 and n_tp == 2 and n_sp > 1 and rest[5].shape[0] <= 33 and cols % (128 * n_sp) == 0 and rest[2].shape[1] == w_query.shape[1] and (
            tokens.shape[1] % (128 * n_sp * n_tp) == 0
        )

    def program(*args):
        body = spread_shards if fits(*args) else shards
        return mapped(body)(*args)

    def mapped(body):
        return jax.shard_map(
            body, mesh=mesh, in_specs=placed, out_specs=P("fs", ("sp", "tp"), None), check_vma=False
        )

    return program
```
